32 devices in a mesh: sp: 8 (over z, y), dp: 4 (over x, core).
Axes of the slice: x: 2, y: 2, z: 4, core: 2. Of those that a mesh axis runs over, the one named last changes fastest.
Arguments:
- residual: bfloat16 [4, 1024, 2048], P('dp', 'sp'), may hold values from -6 to 6
- query_maps: bfloat16 [4, 1024, 2048], P('dp', 'sp'), may hold values from -200 to 200
- key_maps: bfloat16 [4, 1024, 2048], P('dp', 'sp'), may hold values from -200 to 200
- value_rows: bfloat16 [4, 1024, 2048], P('dp', 'sp'), may hold values from -6 to 6
- lambdas: float32 [16], replicated, may hold values from 0.3 to 0.8
- head_gain: float32 [2048], replicated, may hold values from 0.1 to 1.9
- out_weight: bfloat16 [2048, 2048], replicated, may hold values from -0.125 to 0.125
- ffn_gain: float32 [2048], replicated, may hold values from 0.1 to 1.9
- routes: int32 [4, 1024, 2], P('dp', 'sp'), may hold values from 0 to 31, all different within a row; in each aligned block of 128 rows (0 to 127, 128 to 255, ..., all dimensions but the last counted through in order) at most 16 rows name the same one
- route_weights: float32 [4, 1024, 2], P('dp', 'sp'), may hold values from 0.2 to 1
- expert_gate: bfloat16 [32, 2048, 1024], P(('sp', 'dp')), may hold values from -0.125 to 0.125
- expert_up: bfloat16 [32, 2048, 1024], P(('sp', 'dp')), may hold values from -0.125 to 0.125
- expert_down: bfloat16 [32, 1024, 2048], P(('sp', 'dp')), may hold values from -0.1875 to 0.1875
Outputs:
- layer_out: bfloat16 [4, 1024, 2048], P('dp', 'sp')
The draws below stay inside these ranges and needn't reach their ends.
Inputs may be any that keep to these rules, and one draw needn't show every extreme that they name: `routes`: A token's 2 experts differ; among the 128 rows of one device no expert is named more than 16 times, and in every draw some expert is named exactly 16 times by one device's rows.
All inputs are finite; a program needn't handle non-finite values.
Results may differ from the reference program's by a relative error of at most 0.012.
Values may be sent and summed in bfloat16 or wider, within the bound.
A program may use at most 128 MiB of HBM per device.

```python
import math
import jax
import jax.numpy as jnp
import numpy as np
from jax import lax

D = 2048
HEADS = 16
HD = 64
VD = 128
FF = 1024
TOPK = 2
TOK_DEV = 128
SEQ = 1024
EXPERTS = 32
CAP = 16
N_DP = 4


def base_keys(key):
    return 1.3 * jax.random.normal(jax.random.fold_in(key, 11), (N_DP, SEQ, HEADS * 2 * HD), jnp.float32)


def draw_key_maps(key, part):
    drawn = base_keys(key)
    return drawn.astype(jnp.bfloat16)


def draw_query_maps(key, part):
    drawn = 1.3 * jax.random.normal(jax.random.fold_in(key, 21), (N_DP, SEQ, HEADS * 2 * HD), jnp.float32)
    return drawn.astype(jnp.bfloat16)


def shard_levels(key, extent, split, least, largest):
    gain = 1.0
    for axis_at, shards_of in split:
        steps = jax.random.uniform(jax.random.fold_in(jax.random.fold_in(key, 6), axis_at), (shards_of,), jnp.float32, least / len(split), largest / len(split))
        gain = gain * jnp.repeat(jnp.exp(steps), extent[axis_at] // shards_of).reshape((-1,) + (1,) * (len(extent) - 1 - axis_at))
    return gain


def shared_out(own_key, own, number, rows, number_of, top, limit, skew):
    sequence = jax.random.permutation(own_key, number_of)
    crowded, usual = load_shares(number_of, rows * top, limit, skew, True), load_shares(number_of, rows * top, limit, skew, False)
    places = jnp.arange(number_of)

    def named(lengths, turn):
        used = int((lengths > 0).sum())
        fixed = max(1, used // 4)
        passed = fixed + (places - fixed + turn * (used - fixed)) % max(1, number_of - fixed)
        return jnp.zeros((number_of,), jnp.int32).at[sequence[jnp.where(places < fixed, places, passed)]].set(jnp.asarray(lengths, jnp.int32))

    lengths = jnp.where(number % 4 == 0, named(crowded, number // 4), named(usual, number - number // 4 - 1))
    mixed = jax.random.permutation(jax.random.fold_in(own, 3), number_of)
    giver, taker = mixed[0:number_of // 2 * 2:2], mixed[1:number_of // 2 * 2:2]
    slack = jnp.minimum(lengths[giver] - 1, limit - lengths[taker]) // 2
    slack = jnp.where((giver == sequence[0]) | (taker == sequence[0]) | (lengths[taker] == 0), 0, jnp.maximum(slack, 0))
    passed = jax.random.randint(jax.random.fold_in(own, 4), (number_of // 2,), 0, 1 << 20) % (slack + 1)
    lengths = lengths.at[giver].add(-passed).at[taker].add(passed)
    members = jnp.searchsorted(jnp.cumsum(lengths), jnp.arange(rows * top), side="right").astype(jnp.int32)
    table = members.reshape(top, rows).T
    table = table[jax.random.permutation(jax.random.fold_in(own, 1), rows)]
    turn = jax.random.randint(jax.random.fold_in(own, 2), (rows, 1), 0, top)
    return jnp.take_along_axis(table, (jnp.arange(top)[None, :] + turn) % top, axis=1)


def load_shares(count, total, bound, slope, full):
    weights = [(1 << 20) // math.isqrt(rank ** slope) + 1 for rank in range(1, count + 1)]
    largest = bound if full else min(bound, max(-(-total // count), total * weights[0] // sum(weights)))
    least = 1 if total - largest >= count - 1 else 0
    holding, spare = [largest] + [least] * (count - 1), total - largest - least * (count - 1)
    while spare > 0:
        candidates = [i for i in range(1, count) if holding[i] < largest] or [i for i in range(1, count) if holding[i] < bound]
        whole, remaining = sum([weights[i] for i in candidates]), spare
        for i in candidates:
            extra = min(bound - holding[i], max(1, remaining * weights[i] // whole), spare)
            holding[i] = holding[i] + extra
            spare = spare - extra
    return np.array(holding)


def scatter_about(rng, extent, scale, bound, shards=(), kind=jnp.bfloat16):
    gain = shard_levels(rng, extent, shards, -0.22, 0.18) if shards else 1.0
    values = jax.random.normal(rng, extent, jnp.float32) * scale * gain
    return jnp.minimum(jnp.maximum(values, -bound), bound).astype(kind)


def setup_inputs(seed: int = 0) -> dict:
    arg_keys = jax.random.split(jax.random.key(seed), 14)
    residual = scatter_about(arg_keys[0], (N_DP, SEQ, D), 1.0, 6.0, ((0, 4), (1, 8)))
    query_maps = draw_query_maps(jax.random.fold_in(arg_keys[13], 71), 0)
    key_maps = draw_key_maps(jax.random.fold_in(arg_keys[13], 71), 0)
    value_rows = scatter_about(arg_keys[3], (N_DP, SEQ, HEADS * VD), 1.0, 6.0, ((0, 4), (1, 8)))
    lambdas = jnp.clip(jax.random.uniform(arg_keys[4], (HEADS,), jnp.float32, 0.3, 0.8), 0.3, 0.8)
    head_gain = jnp.clip(1.0 + 0.18 * jax.random.normal(arg_keys[5], (HEADS * VD,), jnp.float32), 0.1, 1.9)
    out_weight = scatter_about(arg_keys[6], (HEADS * VD, D), (HEADS * VD) ** -0.5, 0.125)
    ffn_gain = jnp.clip(1.0 + 0.18 * jax.random.normal(arg_keys[7], (D,), jnp.float32), 0.1, 1.9)
    routes_keys = jax.random.split(jax.random.fold_in(arg_keys[8], 1), N_DP * SEQ // TOK_DEV)
    routes_turns = jax.random.permutation(jax.random.fold_in(arg_keys[8], 3), N_DP * SEQ // TOK_DEV)
    routes = jax.vmap(lambda own, number: shared_out(jax.random.fold_in(arg_keys[8], 2), own, number, TOK_DEV, EXPERTS, TOPK, CAP, 2))(routes_keys, routes_turns).reshape((N_DP, SEQ, TOPK))
    route_weights = jnp.clip(jnp.exp(math.log(1.0) - 1.609438 * jax.random.uniform(arg_keys[9], (N_DP, SEQ, TOPK), jnp.float32) ** shard_levels(arg_keys[9], (N_DP, SEQ, TOPK), ((0, 4), (1, 8)), -0.2, 0.2)), 0.2, 1.0)
    expert_gate = scatter_about(arg_keys[10], (EXPERTS, D, FF), D ** -0.5, 0.125, ((0, 32),))
    expert_up = scatter_about(arg_keys[11], (EXPERTS, D, FF), D ** -0.5, 0.125, ((0, 32),))
    expert_down = scatter_about(arg_keys[12], (EXPERTS, FF, D), FF ** -0.5, 0.1875, ((0, 32),))
    return {"residual": residual, "query_maps": query_maps, "key_maps": key_maps, "value_rows": value_rows, "lambdas": lambdas, "head_gain": head_gain, "out_weight": out_weight, "ffn_gain": ffn_gain, "routes": routes, "route_weights": route_weights, "expert_gate": expert_gate, "expert_up": expert_up, "expert_down": expert_down}


eps = 1e-06

def attend_head(query_head, key_head, value_head, lam_head, gain_head):
    length = query_head.shape[0]
    block_rows = min(512, length)
    count_blocks = length // block_rows
    scaling = query_head.shape[-1] ** (-0.5)
    query_blocks = query_head.reshape(count_blocks, block_rows, 2, query_head.shape[-1])
    keys_wide = key_head.astype(jnp.float32)

    def one_block(query_block):
        scores = jnp.einsum('qmd,kmd->mqk', query_block.astype(jnp.float32), keys_wide) * scaling
        probabilities = jax.nn.softmax(scores, axis=-1)
        mixed_map = (probabilities[0] - lam_head * probabilities[1]).astype(jnp.bfloat16)
        head_out = jnp.dot(mixed_map, value_head, preferred_element_type=jnp.float32)
        normed = head_out * lax.rsqrt(lax.optimization_barrier(jnp.mean(head_out * head_out, axis=-1, keepdims=True)) + eps)
        return (normed * gain_head * 0.8).astype(jnp.bfloat16)
    return lax.map(one_block, query_blocks).reshape(length, value_head.shape[-1])

def reference(residual, query_maps, key_maps, value_rows, lambdas, head_gain, out_weight, ffn_gain, routes, route_weights, expert_gate, expert_up, expert_down):
    items = N_DP * HEADS
    query_items = query_maps.reshape(N_DP, SEQ, HEADS, 2, HD).transpose(0, 2, 1, 3, 4).reshape(items, SEQ, 2, HD)
    key_items = key_maps.reshape(N_DP, SEQ, HEADS, 2, HD).transpose(0, 2, 1, 3, 4).reshape(items, SEQ, 2, HD)
    value_items = value_rows.reshape(N_DP, SEQ, HEADS, VD).transpose(0, 2, 1, 3).reshape(items, SEQ, VD)
    lam_items = jnp.tile(lambdas, N_DP)
    gain_items = jnp.tile(head_gain.reshape(HEADS, VD), (N_DP, 1))

    def per_item(packed):
        return attend_head(packed[0], packed[1], packed[2], packed[3], packed[4])
    attended = lax.map(per_item, (query_items, key_items, value_items, lam_items, gain_items))
    attended = attended.reshape(N_DP, HEADS, SEQ, VD).transpose(0, 2, 1, 3).reshape(N_DP * SEQ, HEADS * VD)
    total_rows = N_DP * SEQ
    projected = jnp.dot(attended, out_weight, preferred_element_type=jnp.float32)
    residual_mid = (residual.reshape(total_rows, D).astype(jnp.float32) + projected).astype(jnp.bfloat16)
    middle = residual_mid.astype(jnp.float32)
    expert_input = (middle * lax.rsqrt(lax.optimization_barrier(jnp.mean(middle * middle, axis=-1, keepdims=True)) + eps) * ffn_gain).astype(jnp.bfloat16)
    count_blocks = total_rows // TOK_DEV
    block_routes = routes.reshape(count_blocks, TOK_DEV * TOPK)

    def rank_block(route_block):
        onehot = (route_block[:, None] == jnp.arange(EXPERTS, dtype=jnp.int32)[None, :]).astype(jnp.int32)
        before = jnp.cumsum(onehot, axis=0) - onehot
        return lax.optimization_barrier(jnp.sum(before * onehot, axis=1))
    rank_of = lax.map(rank_block, block_routes).reshape(-1)
    flat_routes = routes.reshape(-1).astype(jnp.int32)
    token_of = (jnp.arange(total_rows * TOPK, dtype=jnp.int32) // TOPK).astype(jnp.int32)
    column = token_of // TOK_DEV * CAP + rank_of
    slot_table = jnp.full((EXPERTS, count_blocks * CAP), total_rows, jnp.int32).at[flat_routes, column].set(token_of)
    weight_table = jnp.zeros((EXPERTS, count_blocks * CAP), jnp.float32).at[flat_routes, column].set(route_weights.reshape(-1))
    padded_input = jnp.concatenate([expert_input, jnp.zeros((1, D), jnp.bfloat16)], axis=0)

    def per_expert(accumulated, packed):
        table_row, weight_row, gate_weight, up_weight, down_weight = packed
        row_block = padded_input[table_row]
        gate_part = jnp.dot(row_block, gate_weight, preferred_element_type=jnp.float32)
        up_part = jnp.dot(row_block, up_weight, preferred_element_type=jnp.float32)
        hidden = (jax.nn.silu(gate_part) * up_part).astype(jnp.bfloat16)
        expert_out = jnp.dot(hidden, down_weight, preferred_element_type=jnp.float32).astype(jnp.bfloat16)
        accumulated = accumulated.at[table_row].add(weight_row[:, None] * expert_out.astype(jnp.float32))
        return (accumulated, None)
    start_sum = jnp.zeros((total_rows + 1, D), jnp.float32)
    accumulated, _ = lax.scan(per_expert, start_sum, (slot_table, weight_table, expert_gate, expert_up, expert_down))
    layer_out = (middle + accumulated[:total_rows]).astype(jnp.bfloat16)
    return layer_out.reshape(N_DP, SEQ, D)
```

```python
import functools
import math

import jax
import jax.numpy as jnp
from jax import lax
from jax.experimental import pallas as pl
from jax.experimental.pallas import tpu as pltpu
from jax.sharding import PartitionSpec as P

D = 2048
HEADS = 16
HD = 64
VD = 128


eps = 1e-06


def attend_head(query_head, key_head, value_head, lam_head, gain_head):
    length = query_head.shape[0]
    block_rows = min(512, length)
    count_blocks = length // block_rows
    scaling = query_head.shape[-1] ** (-0.5)
    query_blocks = query_head.reshape(count_blocks, block_rows, 2, query_head.shape[-1])

    def one_block(query_block):
        scores = (
            jnp.einsum("qmd,kmd->mqk", query_block, key_head, preferred_element_type=jnp.float32)
            * scaling
        )
        probabilities = jax.nn.softmax(scores, axis=-1)
        mixed_map = (probabilities[0] - lam_head * probabilities[1]).astype(jnp.bfloat16)
        head_out = jnp.dot(mixed_map, value_head, preferred_element_type=jnp.float32)
        normed = head_out * lax.rsqrt(jnp.mean(head_out * head_out, axis=-1, keepdims=True) + eps)
        return (normed * gain_head * 0.8).astype(jnp.bfloat16)

    return lax.map(one_block, query_blocks).reshape(length, value_head.shape[-1])


def on_device(
    residual,
    query_maps,
    key_maps,
    value_rows,
    lambdas,
    head_gain,
    out_weight,
    ffn_gain,
    routes,
    route_weights,
    expert_gate,
    expert_up,
    expert_down,
):
    count_sp = lax.axis_size("sp")
    count_dp = lax.axis_size("dp")
    heads_here = HEADS // count_sp
    queries, keys_all, values_all = (
        lax.all_to_all(query_maps, "sp", split_axis=2, concat_axis=1, tiled=True),
        lax.all_to_all(key_maps, "sp", split_axis=2, concat_axis=1, tiled=True),
        lax.all_to_all(value_rows, "sp", split_axis=2, concat_axis=1, tiled=True),
    )
    first_head = lax.axis_index("sp") * heads_here
    lam_here = lax.dynamic_slice_in_dim(lambdas, first_head, heads_here)
    gain_here = lax.dynamic_slice_in_dim(head_gain, first_head * VD, heads_here * VD)
    outputs = []
    for head_index in range(heads_here):
        query_head = queries[0, :, head_index * 2 * HD : (head_index + 1) * 2 * HD].reshape(
            -1, 2, HD
        )
        key_head = keys_all[0, :, head_index * 2 * HD : (head_index + 1) * 2 * HD].reshape(
            -1, 2, HD
        )
        value_head = values_all[0, :, head_index * VD : (head_index + 1) * VD]
        gain_head = gain_here[head_index * VD : (head_index + 1) * VD]
        outputs.append(
            attend_head(query_head, key_head, value_head, lam_here[head_index], gain_head)
        )
    attended = jnp.concatenate(outputs, axis=1)[None]
    returned_heads = lax.all_to_all(attended, "sp", split_axis=1, concat_axis=2, tiled=True)
    projected = jnp.dot(returned_heads[0], out_weight, preferred_element_type=jnp.float32)
    residual_mid = (residual[0].astype(jnp.float32) + projected).astype(jnp.bfloat16)
    middle = residual_mid.astype(jnp.float32)
    expert_input = (
        middle * lax.rsqrt(jnp.mean(middle * middle, axis=-1, keepdims=True) + eps) * ffn_gain
    ).astype(jnp.bfloat16)
    tok_rows = residual.shape[1]
    experts_all = count_sp * count_dp
    capacity = max(2, 4 * tok_rows // experts_all)
    flat_routes = routes[0].reshape(-1)
    flat_weights = route_weights[0].reshape(-1)
    onehot = (flat_routes[:, None] == jnp.arange(experts_all, dtype=jnp.int32)[None, :]).astype(
        jnp.int32
    )
    before = jnp.cumsum(onehot, axis=0) - onehot
    rank_of = jnp.sum(before * onehot, axis=1)
    slot = flat_routes * capacity + rank_of
    token_of = jnp.arange(flat_routes.shape[0], dtype=jnp.int32) // routes.shape[2]
    slot_token = jnp.full((experts_all * capacity,), tok_rows, jnp.int32).at[slot].set(token_of)
    padded_input = jnp.concatenate([expert_input, jnp.zeros((1, D), jnp.bfloat16)], axis=0)
    buffer = padded_input[slot_token].reshape(experts_all, capacity, D)
    received = lax.all_to_all(buffer, ("sp", "dp"), split_axis=0, concat_axis=0, tiled=True)
    row_block = received.reshape(-1, D)
    gate_part = jnp.dot(row_block, expert_gate[0], preferred_element_type=jnp.float32)
    up_part = jnp.dot(row_block, expert_up[0], preferred_element_type=jnp.float32)
    hidden = (jax.nn.silu(gate_part) * up_part).astype(jnp.bfloat16)
    expert_out = jnp.dot(hidden, expert_down[0], preferred_element_type=jnp.float32).astype(
        jnp.bfloat16
    )
    returned = lax.all_to_all(
        expert_out.reshape(received.shape), ("sp", "dp"), split_axis=0, concat_axis=0, tiled=True
    )
    picked = returned.reshape(experts_all * capacity, D)[slot]
    weighted = (picked.astype(jnp.float32) * flat_weights[:, None]).reshape(
        tok_rows, routes.shape[2], D
    )
    layer_out = (middle + jnp.sum(weighted, axis=1)).astype(jnp.bfloat16)
    return layer_out[None]


MESH = pl.DeviceIdType.MESH
VMEM_LIMIT = 60 * 1024 * 1024


def slot_masks(routes_ref, experts_all, capacity):
    rows = routes_ref.shape[0]
    first, second = routes_ref[:, 0:1], routes_ref[:, 1:2]
    experts = lax.broadcasted_iota(jnp.int32, (rows, experts_all), 1)
    named_first, named_second = experts == first, experts == second
    named = jnp.where(named_first | named_second, 1.0, 0.0).astype(jnp.bfloat16)
    earlier = lax.broadcasted_iota(jnp.int32, (rows, rows), 0) > lax.broadcasted_iota(
        jnp.int32, (rows, rows), 1
    )
    before = jnp.dot(
        jnp.where(earlier, 1.0, 0.0).astype(jnp.bfloat16), named, preferred_element_type=jnp.float32
    )
    slots = lax.broadcasted_iota(jnp.int32, (rows, experts_all * capacity), 1)
    masks = []
    for route, chosen in ((first, named_first), (second, named_second)):
        rank = jnp.sum(jnp.where(chosen, before, 0.0), axis=1, keepdims=True).astype(jnp.int32)
        masks.append(slots == route * capacity + rank)
    return masks


def mixer_kernel(
    count_sp,
    experts_all,
    capacity,
    lam_ref,
    q_ref,
    k_ref,
    v_ref,
    residual_ref,
    gain_ref,
    ow_hbm,
    fgain_ref,
    routes_ref,
    mid_ref,
    buf_ref,
    qh,
    kh,
    vh,
    outs,
    att,
    ow,
    xin,
    send_sem,
    recv_sem,
    back_send,
    back_recv,
    local_sem,
    ow_sem,
):
    me = lax.axis_index("sp")
    rows = q_ref.shape[0]
    heads_here = HEADS // count_sp
    length = rows * count_sp
    sources = ((k_ref, kh), (q_ref, qh), (v_ref, vh))

    barrier = pltpu.get_barrier_semaphore()

    def greet(d, carry):
        pl.semaphore_signal(
            barrier, inc=1, device_id={"sp": lax.rem(me + d, count_sp)}, device_id_type=MESH
        )
        return carry

    lax.fori_loop(1, count_sp, greet, 0)
    weight_copy = pltpu.make_async_copy(ow_hbm, ow, ow_sem)
    my_rows = pl.ds(pl.multiple_of(me * rows, rows), rows)

    def local_copy(t, h):
        src, dst = sources[t]
        cols = pl.ds(pl.multiple_of((me * heads_here + h) * VD, VD), VD)
        return pltpu.make_async_copy(src.at[:, cols], dst.at[h, my_rows, :], local_sem.at[t, h])

    def outgoing(t, h, d):
        src, dst = sources[t]
        peer = lax.rem(me + d, count_sp)
        cols = pl.ds(pl.multiple_of((peer * heads_here + h) * VD, VD), VD)
        return pltpu.make_async_remote_copy(
            src_ref=src.at[:, cols],
            dst_ref=dst.at[h, my_rows, :],
            send_sem=send_sem.at[t, h, d],
            recv_sem=recv_sem.at[t, h, d],
            device_id={"sp": peer},
            device_id_type=MESH,
        )

    pl.semaphore_wait(barrier, count_sp - 1)
    for h in range(heads_here):

        def start_all(i, carry, h=h):
            d = 1 + lax.rem(i + count_sp // 2 - 1, count_sp - 1)
            for t in range(3):
                outgoing(t, h, d).start()
            return carry

        lax.fori_loop(0, count_sp - 1, start_all, 0)
        for t in range(3):
            local_copy(t, h).start()
    weight_copy.start()

    def returning(h, p, d):
        dst_cols = pl.ds(pl.multiple_of((me * heads_here + h) * VD, VD), VD)
        return pltpu.make_async_remote_copy(
            src_ref=outs.at[h, pl.ds(pl.multiple_of(p * rows, rows), rows), :],
            dst_ref=att.at[:, dst_cols],
            send_sem=back_send.at[h, d],
            recv_sem=back_recv.at[h, d],
            device_id={"sp": p},
            device_id_type=MESH,
        )

    factor = HD ** (-0.5) * math.log2(math.e)
    lanes = lax.broadcasted_iota(jnp.int32, (rows, VD), 1)
    for h in range(heads_here):
        for t in range(3):
            local_copy(t, h).wait()

            def arrived(d, carry, t=t, h=h):
                outgoing(t, h, d).wait_recv()
                return carry

            lax.fori_loop(1, count_sp, arrived, 0)
        head = me * heads_here + h
        lam = lam_ref[head]
        gain = gain_ref[pl.ds(head, 1), :]

        def attend(p, h=h, lam=lam, gain=gain):
            at = pl.ds(pl.multiple_of(p * rows, rows), rows)
            q = qh[h, at, :]
            zero = jnp.zeros_like(q)
            both = jnp.concatenate(
                [jnp.where(lanes < HD, q, zero), jnp.where(lanes < HD, zero, q)], axis=0
            )
            scores = lax.dot_general(
                both, kh[h], (((1,), (1,)), ((), ())), preferred_element_type=jnp.float32
            )
            top = jnp.max(scores, axis=1, keepdims=True)
            e = jnp.exp2((scores - top) * factor)
            total = jnp.sum(e, axis=1, keepdims=True)
            total_1, total_2 = total[:rows], total[rows:]
            share = lam * total_1 / total_2
            mixed = (e[:rows] - share * e[rows:]).astype(jnp.bfloat16)
            head_out = jnp.dot(mixed, vh[h], preferred_element_type=jnp.float32) / total_1
            normed = head_out * lax.rsqrt(
                jnp.mean(head_out * head_out, axis=-1, keepdims=True) + eps
            )
            return (normed * gain * 0.8).astype(jnp.bfloat16)

        def step(i, carry, h=h, attend=attend):
            d = 1 + lax.rem(i + count_sp // 2 - 1, count_sp - 1)
            p = lax.rem(me + d, count_sp)
            outs[h, pl.ds(pl.multiple_of(p * rows, rows), rows), :] = attend(p)
            returning(h, p, d).start()
            return carry

        lax.fori_loop(0, count_sp - 1, step, 0)
        att[:, pl.ds(pl.multiple_of(head * VD, VD), VD)] = attend(me)

    masks = slot_masks(routes_ref, experts_all, capacity)
    dispatch = jnp.where(masks[0] | masks[1], 1.0, 0.0).T.astype(jnp.bfloat16)
    weight_copy.wait()
    for h in range(heads_here):

        def back(d, carry, h=h):
            returning(h, lax.rem(me + d, count_sp), d).wait_recv()
            return carry

        lax.fori_loop(1, count_sp, back, 0)

    tile = 512
    square = jnp.zeros((rows, 1), jnp.float32)
    for j in range(D // tile):
        cols = slice(j * tile, (j + 1) * tile)
        projected = jnp.dot(att[...], ow[:, cols], preferred_element_type=jnp.float32)
        middle = (residual_ref[:, cols].astype(jnp.float32) + projected).astype(jnp.bfloat16)
        mid_ref[:, cols] = middle
        wide = middle.astype(jnp.float32)
        square = square + jnp.sum(wide * wide, axis=1, keepdims=True)
    scale = lax.rsqrt(square / D + eps)
    xin[...] = (mid_ref[...].astype(jnp.float32) * scale * fgain_ref[...]).astype(jnp.bfloat16)
    for j in range(D // tile):
        cols = slice(j * tile, (j + 1) * tile)
        buf_ref[:, cols] = jnp.dot(
            dispatch, xin[:, cols], preferred_element_type=jnp.float32
        ).astype(jnp.bfloat16)

    for h in range(heads_here):

        def drain(d, carry, h=h):
            for t in range(3):
                outgoing(t, h, d).wait_send()
            returning(h, lax.rem(me + d, count_sp), d).wait_send()
            return carry

        lax.fori_loop(1, count_sp, drain, 0)


def experts_kernel(
    count_sp,
    count_dp,
    capacity,
    buf_ref,
    mid_ref,
    routes_ref,
    weights_ref,
    gate_hbm,
    up_hbm,
    down_hbm,
    out_ref,
    received,
    results,
    returned,
    gate,
    up,
    down,
    hidden,
    send_sem,
    recv_sem,
    back_send,
    back_recv,
    local_sem,
    weight_sem,
):
    count = count_sp * count_dp
    me = lax.axis_index("sp") * count_dp + lax.axis_index("dp")
    width = gate.shape[1]

    def coords(p):
        return {"sp": p // count_dp, "dp": lax.rem(p, count_dp)}

    barrier = pltpu.get_barrier_semaphore()

    def greet(d, carry):
        pl.semaphore_signal(
            barrier, inc=1, device_id=coords(lax.rem(me + d, count)), device_id_type=MESH
        )
        return carry

    lax.fori_loop(1, count, greet, 0)

    def rows_of(i):
        return pl.ds(pl.multiple_of(i * capacity, capacity), capacity)

    def offset(i):
        return 1 + lax.rem(i + count // 2 - 2, count - 1)

    def outgoing(i):
        p = lax.rem(me + offset(i), count)
        return pltpu.make_async_remote_copy(
            src_ref=buf_ref.at[rows_of(p), :],
            dst_ref=received.at[rows_of(i), :],
            send_sem=send_sem.at[i],
            recv_sem=recv_sem.at[i],
            device_id=coords(p),
            device_id_type=MESH,
        )

    def returning(i):
        p = lax.rem(me + count - offset(i), count)
        return pltpu.make_async_remote_copy(
            src_ref=results.at[rows_of(i), :],
            dst_ref=returned.at[rows_of(me), :],
            send_sem=back_send.at[i],
            recv_sem=back_recv.at[i],
            device_id=coords(p),
            device_id_type=MESH,
        )

    own_in = pltpu.make_async_copy(
        buf_ref.at[rows_of(me), :], received.at[rows_of(0), :], local_sem.at[0]
    )
    own_out = pltpu.make_async_copy(
        results.at[rows_of(0), :], returned.at[rows_of(me), :], local_sem.at[1]
    )
    loads = [
        pltpu.make_async_copy(src, dst, weight_sem.at[j])
        for j, (src, dst) in enumerate(((gate_hbm, gate), (up_hbm, up), (down_hbm, down)))
    ]
    pl.semaphore_wait(barrier, count - 1)

    def start(i, carry):
        outgoing(i).start()
        return carry

    lax.fori_loop(1, count, start, 0)
    own_in.start()
    for load in loads:
        load.start()

    masks = slot_masks(routes_ref, count, capacity)
    combine = jnp.where(masks[0], weights_ref[:, 0:1], 0.0) + jnp.where(
        masks[1], weights_ref[:, 1:2], 0.0
    )
    combine_high = combine.astype(jnp.bfloat16)
    combine_low = (combine - combine_high.astype(jnp.float32)).astype(jnp.bfloat16)

    own_in.wait()
    for load in loads:
        load.wait()
    chunks = 4
    per_chunk = count // chunks
    chunk_rows = per_chunk * capacity

    def chunk(c, carry):
        def arrived(i, carry):
            @pl.when(i > 0)
            def _():
                outgoing(i).wait_recv()

            return carry

        lax.fori_loop(c * per_chunk, (c + 1) * per_chunk, arrived, 0)
        at = pl.ds(pl.multiple_of(c * chunk_rows, chunk_rows), chunk_rows)

        def make_hidden(j, carry):
            cols = pl.ds(pl.multiple_of(j * 256, 256), 256)
            gate_part = jnp.dot(received[at, :], gate[:, cols], preferred_element_type=jnp.float32)
            up_part = jnp.dot(received[at, :], up[:, cols], preferred_element_type=jnp.float32)
            hidden[:, cols] = (jax.nn.silu(gate_part) * up_part).astype(jnp.bfloat16)
            return carry

        lax.fori_loop(0, width // 256, make_hidden, 0)

        def make_out(j, carry):
            cols = pl.ds(pl.multiple_of(j * 512, 512), 512)
            results[at, cols] = jnp.dot(
                hidden[...], down[:, cols], preferred_element_type=jnp.float32
            ).astype(jnp.bfloat16)
            return carry

        lax.fori_loop(0, D // 512, make_out, 0)

        def send_back(i, carry):
            @pl.when(i > 0)
            def _():
                returning(i).start()

            @pl.when(i == 0)
            def _():
                own_out.start()

            return carry

        lax.fori_loop(c * per_chunk, (c + 1) * per_chunk, send_back, 0)
        return carry

    lax.fori_loop(0, chunks, chunk, 0)
    own_out.wait()

    def back(i, carry):
        returning(i).wait_recv()
        return carry

    lax.fori_loop(1, count, back, 0)
    for j in range(D // 512):
        cols = slice(j * 512, (j + 1) * 512)
        block = returned[:, cols]
        added = jnp.dot(combine_high, block, preferred_element_type=jnp.float32) + jnp.dot(
            combine_low, block, preferred_element_type=jnp.float32
        )
        out_ref[:, cols] = (mid_ref[:, cols].astype(jnp.float32) + added).astype(jnp.bfloat16)

    def drain(i, carry):
        outgoing(i).wait_send()
        returning(i).wait_send()
        return carry

    lax.fori_loop(1, count, drain, 0)


def kernels_on_device(
    residual,
    query_maps,
    key_maps,
    value_rows,
    lambdas,
    head_gain,
    out_weight,
    ffn_gain,
    routes,
    route_weights,
    expert_gate,
    expert_up,
    expert_down,
):
    count_sp = lax.axis_size("sp")
    count_dp = lax.axis_size("dp")
    experts_all = count_sp * count_dp
    rows = residual.shape[1]
    capacity = max(2, 4 * rows // experts_all)
    if capacity % 16:
        return on_device(
            residual,
            query_maps,
            key_maps,
            value_rows,
            lambdas,
            head_gain,
            out_weight,
            ffn_gain,
            routes,
            route_weights,
            expert_gate,
            expert_up,
            expert_down,
        )
    heads_here = HEADS // count_sp
    slots = experts_all * capacity
    vmem = pl.BlockSpec(memory_space=pltpu.VMEM)
    hbm = pl.BlockSpec(memory_space=pl.ANY)
    dma = pltpu.SemaphoreType.DMA
    bf16 = jnp.bfloat16
    length = rows * count_sp
    middle, buffer = pl.pallas_call(
        functools.partial(mixer_kernel, count_sp, experts_all, capacity),
        out_shape=(
            jax.ShapeDtypeStruct((rows, D), bf16),
            jax.ShapeDtypeStruct((slots, D), bf16),
        ),
        in_specs=[pl.BlockSpec(memory_space=pltpu.SMEM), hbm, hbm, hbm, vmem, vmem, hbm, vmem, vmem],
        out_specs=(vmem, vmem),
        scratch_shapes=[
            pltpu.VMEM((heads_here, length, VD), bf16),
            pltpu.VMEM((heads_here, length, VD), bf16),
            pltpu.VMEM((heads_here, length, VD), bf16),
            pltpu.VMEM((heads_here, length, VD), bf16),
            pltpu.VMEM((rows, HEADS * VD), bf16),
            pltpu.VMEM(out_weight.shape, bf16),
            pltpu.VMEM((rows, D), bf16),
            dma((3, heads_here, count_sp)),
            dma((3, heads_here, count_sp)),
            dma((heads_here, count_sp)),
            dma((heads_here, count_sp)),
            dma((3, heads_here)),
            dma,
        ],
        compiler_params=pltpu.CompilerParams(
            collective_id=0, has_side_effects=True, vmem_limit_bytes=VMEM_LIMIT
        ),
    )(
        lambdas,
        query_maps[0],
        key_maps[0],
        value_rows[0],
        residual[0],
        head_gain.reshape(HEADS, VD),
        out_weight,
        ffn_gain.reshape(1, D),
        routes[0],
    )
    width = expert_gate.shape[2]
    out = pl.pallas_call(
        functools.partial(experts_kernel, count_sp, count_dp, capacity),
        out_shape=jax.ShapeDtypeStruct((rows, D), bf16),
        in_specs=[hbm, vmem, vmem, vmem, hbm, hbm, hbm],
        out_specs=vmem,
        scratch_shapes=[
            pltpu.VMEM((slots, D), bf16),
            pltpu.VMEM((slots, D), bf16),
            pltpu.VMEM((slots, D), bf16),
            pltpu.VMEM((D, width), bf16),
            pltpu.VMEM((D, width), bf16),
            pltpu.VMEM((width, D), bf16),
            pltpu.VMEM((slots // 4, width), bf16),
            dma((experts_all,)),
            dma((experts_all,)),
            dma((experts_all,)),
            dma((experts_all,)),
            dma((2,)),
            dma((3,)),
        ],
        compiler_params=pltpu.CompilerParams(
            collective_id=1, has_side_effects=True, vmem_limit_bytes=VMEM_LIMIT
        ),
    )(buffer, middle, routes[0], route_weights[0], expert_gate[0], expert_up[0], expert_down[0])
    return out[None]


def solution(mesh):
    return jax.shard_map(
        kernels_on_device,
        mesh=mesh,
        in_specs=(
            P("dp", "sp", None),
            P("dp", "sp", None),
            P("dp", "sp", None),
            P("dp", "sp", None),
            P(),
            P(),
            P(),
            P(),
            P("dp", "sp", None),
            P("dp", "sp", None),
            P(("sp", "dp"), None, None),
            P(("sp", "dp"), None, None),
            P(("sp", "dp"), None, None),
        ),
        out_specs=P("dp", "sp", None),
        check_vma=False,
    )
```

```python
import functools
import math

import jax
import jax.numpy as jnp
from jax import lax
from jax.experimental import pallas as pl
from jax.experimental.pallas import tpu as pltpu
from jax.sharding import PartitionSpec as P

D = 2048
HEADS = 16
HD = 64
VD = 128


eps = 1e-06


def attend_head(query_head, key_head, value_head, lam_head, gain_head):
    length = query_head.shape[0]
    block_rows = min(512, length)
    count_blocks = length // block_rows
    scaling = query_head.shape[-1] ** (-0.5)
    query_blocks = query_head.reshape(count_blocks, block_rows, 2, query_head.shape[-1])

    def one_block(query_block):
        scores = (
            jnp.einsum("qmd,kmd->mqk", query_block, key_head, preferred_element_type=jnp.float32)
            * scaling
        )
        probabilities = jax.nn.softmax(scores, axis=-1)
        mixed_map = (probabilities[0] - lam_head * probabilities[1]).astype(jnp.bfloat16)
        head_out = jnp.dot(mixed_map, value_head, preferred_element_type=jnp.float32)
        normed = head_out * lax.rsqrt(jnp.mean(head_out * head_out, axis=-1, keepdims=True) + eps)
        return (normed * gain_head * 0.8).astype(jnp.bfloat16)

    return lax.map(one_block, query_blocks).reshape(length, value_head.shape[-1])


def on_device(
    residual,
    query_maps,
    key_maps,
    value_rows,
    lambdas,
    head_gain,
    out_weight,
    ffn_gain,
    routes,
    route_weights,
    expert_gate,
    expert_up,
    expert_down,
):
    count_sp = lax.axis_size("sp")
    count_dp = lax.axis_size("dp")
    heads_here = HEADS // count_sp
    queries, keys_all, values_all = (
        lax.all_to_all(query_maps, "sp", split_axis=2, concat_axis=1, tiled=True),
        lax.all_to_all(key_maps, "sp", split_axis=2, concat_axis=1, tiled=True),
        lax.all_to_all(value_rows, "sp", split_axis=2, concat_axis=1, tiled=True),
    )
    first_head = lax.axis_index("sp") * heads_here
    lam_here = lax.dynamic_slice_in_dim(lambdas, first_head, heads_here)
    gain_here = lax.dynamic_slice_in_dim(head_gain, first_head * VD, heads_here * VD)
    outputs = []
    for head_index in range(heads_here):
        query_head = queries[0, :, head_index * 2 * HD : (head_index + 1) * 2 * HD].reshape(
            -1, 2, HD
        )
        key_head = keys_all[0, :, head_index * 2 * HD : (head_index + 1) * 2 * HD].reshape(
            -1, 2, HD
        )
        value_head = values_all[0, :, head_index * VD : (head_index + 1) * VD]
        gain_head = gain_here[head_index * VD : (head_index + 1) * VD]
        outputs.append(
            attend_head(query_head, key_head, value_head, lam_here[head_index], gain_head)
        )
    attended = jnp.concatenate(outputs, axis=1)[None]
    returned_heads = lax.all_to_all(attended, "sp", split_axis=1, concat_axis=2, tiled=True)
    projected = jnp.dot(returned_heads[0], out_weight, preferred_element_type=jnp.float32)
    residual_mid = (residual[0].astype(jnp.float32) + projected).astype(jnp.bfloat16)
    middle = residual_mid.astype(jnp.float32)
    expert_input = (
        middle * lax.rsqrt(jnp.mean(middle * middle, axis=-1, keepdims=True) + eps) * ffn_gain
    ).astype(jnp.bfloat16)
    tok_rows = residual.shape[1]
    experts_all = count_sp * count_dp
    capacity = max(2, 4 * tok_rows // experts_all)
    flat_routes = routes[0].reshape(-1)
    flat_weights = route_weights[0].reshape(-1)
    onehot = (flat_routes[:, None] == jnp.arange(experts_all, dtype=jnp.int32)[None, :]).astype(
        jnp.int32
    )
    before = jnp.cumsum(onehot, axis=0) - onehot
    rank_of = jnp.sum(before * onehot, axis=1)
    slot = flat_routes * capacity + rank_of
    token_of = jnp.arange(flat_routes.shape[0], dtype=jnp.int32) // routes.shape[2]
    slot_token = jnp.full((experts_all * capacity,), tok_rows, jnp.int32).at[slot].set(token_of)
    padded_input = jnp.concatenate([expert_input, jnp.zeros((1, D), jnp.bfloat16)], axis=0)
    buffer = padded_input[slot_token].reshape(experts_all, capacity, D)
    received = lax.all_to_all(buffer, ("sp", "dp"), split_axis=0, concat_axis=0, tiled=True)
    row_block = received.reshape(-1, D)
    gate_part = jnp.dot(row_block, expert_gate[0], preferred_element_type=jnp.float32)
    up_part = jnp.dot(row_block, expert_up[0], preferred_element_type=jnp.float32)
    hidden = (jax.nn.silu(gate_part) * up_part).astype(jnp.bfloat16)
    expert_out = jnp.dot(hidden, expert_down[0], preferred_element_type=jnp.float32).astype(
        jnp.bfloat16
    )
    returned = lax.all_to_all(
        expert_out.reshape(received.shape), ("sp", "dp"), split_axis=0, concat_axis=0, tiled=True
    )
    picked = returned.reshape(experts_all * capacity, D)[slot]
    weighted = (picked.astype(jnp.float32) * flat_weights[:, None]).reshape(
        tok_rows, routes.shape[2], D
    )
    layer_out = (middle + jnp.sum(weighted, axis=1)).astype(jnp.bfloat16)
    return layer_out[None]


MESH = pl.DeviceIdType.MESH
VMEM_LIMIT = 60 * 1024 * 1024


def slot_masks(routes, first_expert, experts_all, experts_here, capacity):
    rows = routes.shape[1]
    first, second = routes[0:1, :], routes[1:2, :]
    experts = lax.broadcasted_iota(jnp.int32, (experts_all, rows), 0)
    named_first, named_second = experts == first, experts == second
    named = jnp.where(named_first | named_second, 1.0, 0.0).astype(jnp.bfloat16)
    earlier = lax.broadcasted_iota(jnp.int32, (rows, rows), 0) < lax.broadcasted_iota(
        jnp.int32, (rows, rows), 1
    )
    before = jnp.dot(
        named, jnp.where(earlier, 1.0, 0.0).astype(jnp.bfloat16), preferred_element_type=jnp.float32
    )
    slots = lax.broadcasted_iota(jnp.int32, (experts_here * capacity, rows), 0)
    masks = []
    for route, chosen in ((first, named_first), (second, named_second)):
        rank = jnp.sum(jnp.where(chosen, before, 0.0), axis=0, keepdims=True).astype(jnp.int32)
        masks.append(slots == (route - first_expert) * capacity + rank)
    return masks


def mixer_kernel(
    count_sp,
    lam_ref,
    q_ref,
    k_ref,
    v_ref,
    residual_ref,
    gain_ref,
    ow_hbm,
    fgain_ref,
    mid_ref,
    xin_ref,
    qh,
    kh,
    vh,
    outs,
    att,
    ow,
    send_sem,
    recv_sem,
    back_send,
    back_recv,
    local_sem,
    ow_sem,
):
    me = lax.axis_index("sp")
    rows = q_ref.shape[0]
    heads_here = HEADS // count_sp
    length = rows * count_sp
    sources = ((k_ref, kh), (q_ref, qh), (v_ref, vh))

    barrier = pltpu.get_barrier_semaphore()

    def greet(d, carry):
        pl.semaphore_signal(
            barrier, inc=1, device_id={"sp": lax.rem(me + d, count_sp)}, device_id_type=MESH
        )
        return carry

    lax.fori_loop(1, count_sp, greet, 0)
    weight_copy = pltpu.make_async_copy(ow_hbm, ow, ow_sem)
    my_rows = pl.ds(pl.multiple_of(me * rows, rows), rows)

    def local_copy(t, h):
        src, dst = sources[t]
        cols = pl.ds(pl.multiple_of((me * heads_here + h) * VD, VD), VD)
        return pltpu.make_async_copy(src.at[:, cols], dst.at[h, my_rows, :], local_sem.at[t, h])

    def outgoing(t, h, d):
        src, dst = sources[t]
        peer = lax.rem(me + d, count_sp)
        cols = pl.ds(pl.multiple_of((peer * heads_here + h) * VD, VD), VD)
        return pltpu.make_async_remote_copy(
            src_ref=src.at[:, cols],
            dst_ref=dst.at[h, my_rows, :],
            send_sem=send_sem.at[t, h, d],
            recv_sem=recv_sem.at[t, h, d],
            device_id={"sp": peer},
            device_id_type=MESH,
        )

    pl.semaphore_wait(barrier, count_sp - 1)
    for h in range(heads_here):

        def start_all(i, carry, h=h):
            d = 1 + lax.rem(i + count_sp // 2 - 1, count_sp - 1)
            for t in range(3):
                outgoing(t, h, d).start()
            return carry

        lax.fori_loop(0, count_sp - 1, start_all, 0)
        for t in range(3):
            local_copy(t, h).start()
    weight_copy.start()

    def returning(h, p, d):
        dst_cols = pl.ds(pl.multiple_of((me * heads_here + h) * VD, VD), VD)
        return pltpu.make_async_remote_copy(
            src_ref=outs.at[h, pl.ds(pl.multiple_of(p * rows, rows), rows), :],
            dst_ref=att.at[:, dst_cols],
            send_sem=back_send.at[h, d],
            recv_sem=back_recv.at[h, d],
            device_id={"sp": p},
            device_id_type=MESH,
        )

    factor = HD ** (-0.5) * math.log2(math.e)
    lanes = lax.broadcasted_iota(jnp.int32, (rows, VD), 1)
    for h in range(heads_here):
        for t in range(3):
            local_copy(t, h).wait()

            def arrived(d, carry, t=t, h=h):
                outgoing(t, h, d).wait_recv()
                return carry

            lax.fori_loop(1, count_sp, arrived, 0)
        head = me * heads_here + h
        lam = lam_ref[head]
        gain = gain_ref[pl.ds(head, 1), :]

        def attend(p, h=h, lam=lam, gain=gain):
            at = pl.ds(pl.multiple_of(p * rows, rows), rows)
            q = qh[h, at, :]
            zero = jnp.zeros_like(q)
            both = jnp.concatenate(
                [jnp.where(lanes < HD, q, zero), jnp.where(lanes < HD, zero, q)], axis=0
            )
            scores = lax.dot_general(
                both, kh[h], (((1,), (1,)), ((), ())), preferred_element_type=jnp.float32
            )
            top = jnp.max(scores, axis=1, keepdims=True)
            e = jnp.exp2((scores - top) * factor)
            total = jnp.sum(e, axis=1, keepdims=True)
            total_1, total_2 = total[:rows], total[rows:]
            share = lam * total_1 / total_2
            mixed = (e[:rows] - share * e[rows:]).astype(jnp.bfloat16)
            head_out = jnp.dot(mixed, vh[h], preferred_element_type=jnp.float32) / total_1
            normed = head_out * lax.rsqrt(
                jnp.mean(head_out * head_out, axis=-1, keepdims=True) + eps
            )
            return (normed * gain * 0.8).astype(jnp.bfloat16)

        def step(i, carry, h=h, attend=attend):
            d = 1 + lax.rem(i + count_sp // 2 - 1, count_sp - 1)
            p = lax.rem(me + d, count_sp)
            outs[h, pl.ds(pl.multiple_of(p * rows, rows), rows), :] = attend(p)
            returning(h, p, d).start()
            return carry

        lax.fori_loop(0, count_sp - 1, step, 0)
        att[:, pl.ds(pl.multiple_of(head * VD, VD), VD)] = attend(me)

    weight_copy.wait()
    for h in range(heads_here):

        def back(d, carry, h=h):
            returning(h, lax.rem(me + d, count_sp), d).wait_recv()
            return carry

        lax.fori_loop(1, count_sp, back, 0)

    tile = 512
    square = jnp.zeros((rows, 1), jnp.float32)
    for j in range(D // tile):
        cols = slice(j * tile, (j + 1) * tile)
        projected = jnp.dot(att[...], ow[:, cols], preferred_element_type=jnp.float32)
        middle = (residual_ref[:, cols].astype(jnp.float32) + projected).astype(jnp.bfloat16)
        mid_ref[:, cols] = middle
        wide = middle.astype(jnp.float32)
        square = square + jnp.sum(wide * wide, axis=1, keepdims=True)
    scale = lax.rsqrt(square / D + eps)
    xin_ref[...] = (mid_ref[...].astype(jnp.float32) * scale * fgain_ref[...]).astype(jnp.bfloat16)

    for h in range(heads_here):

        def drain(d, carry, h=h):
            for t in range(3):
                outgoing(t, h, d).wait_send()
            returning(h, lax.rem(me + d, count_sp), d).wait_send()
            return carry

        lax.fori_loop(1, count_sp, drain, 0)


PARTS = 2


def experts_kernel(
    count_sp,
    count_dp,
    capacity,
    xin_ref,
    mid_ref,
    routes_ref,
    weights_ref,
    gate_hbm,
    up_hbm,
    down_hbm,
    out_ref,
    routes_far,
    weights_far,
    xin_far,
    partial,
    far_sum,
    buffer,
    received,
    results,
    returned,
    gate,
    up,
    down,
    hidden,
    far_send,
    far_recv,
    sum_send,
    sum_recv,
    send_sem,
    recv_sem,
    back_send,
    back_recv,
    own_sem,
    weight_sem,
):
    count = count_sp * count_dp
    half = count // 2
    sp = lax.axis_index("sp")
    base = (sp // (count_sp // 2)) * half
    me = sp * count_dp + lax.axis_index("dp") - base
    partner = {"sp": lax.rem(sp + count_sp // 2, count_sp)}
    width = gate.shape[1]
    span = D // PARTS

    def coords(p):
        return {"sp": (base + p) // count_dp, "dp": lax.rem(base + p, count_dp)}

    barrier = pltpu.get_barrier_semaphore()

    def greet(d, carry):
        pl.semaphore_signal(
            barrier, inc=1, device_id=coords(lax.rem(me + d, half)), device_id_type=MESH
        )
        return carry

    lax.fori_loop(1, half, greet, 0)
    pl.semaphore_signal(barrier, inc=1, device_id=partner, device_id_type=MESH)

    def rows_of(b, i):
        return pl.ds(pl.multiple_of((b * half + i) * capacity, capacity), capacity)

    def part(c):
        return pl.ds(c * span, span)

    def offset(i):
        return 1 + lax.rem(i + half // 2 - 2, half - 1)

    def to_partner(src, dst, sent, got):
        return pltpu.make_async_remote_copy(
            src_ref=src,
            dst_ref=dst,
            send_sem=sent,
            recv_sem=got,
            device_id=partner,
            device_id_type=MESH,
        )

    far = [
        to_partner(xin_ref.at[:, part(c)], xin_far.at[:, part(c)], far_send.at[c], far_recv.at[c])
        for c in range(PARTS)
    ]
    far.append(to_partner(routes_ref, routes_far, far_send.at[PARTS], far_recv.at[PARTS]))
    far.append(
        to_partner(weights_ref, weights_far, far_send.at[PARTS + 1], far_recv.at[PARTS + 1])
    )
    far_back = [
        to_partner(partial.at[:, part(c)], far_sum.at[:, part(c)], sum_send.at[c], sum_recv.at[c])
        for c in range(PARTS)
    ]

    def outgoing(b, c, i):
        p = lax.rem(me + offset(i), half)
        return pltpu.make_async_remote_copy(
            src_ref=buffer.at[rows_of(b, p), part(c)],
            dst_ref=received.at[rows_of(b, i), part(c)],
            send_sem=send_sem.at[b, c, i],
            recv_sem=recv_sem.at[b, c, i],
            device_id=coords(p),
            device_id_type=MESH,
        )

    def returning(b, c, i):
        p = lax.rem(me + half - offset(i), half)
        return pltpu.make_async_remote_copy(
            src_ref=results.at[rows_of(b, i), part(c)],
            dst_ref=returned.at[rows_of(b, me), part(c)],
            send_sem=back_send.at[b, c, i],
            recv_sem=back_recv.at[b, c, i],
            device_id=coords(p),
            device_id_type=MESH,
        )

    def own_in(b, c):
        return pltpu.make_async_copy(
            buffer.at[rows_of(b, me), part(c)],
            received.at[rows_of(b, 0), part(c)],
            own_sem.at[0, b, c],
        )

    def own_out(b, c):
        return pltpu.make_async_copy(
            results.at[rows_of(b, 0), part(c)],
            returned.at[rows_of(b, me), part(c)],
            own_sem.at[1, b, c],
        )

    loads = [
        pltpu.make_async_copy(src, dst, weight_sem.at[j])
        for j, (src, dst) in enumerate(((gate_hbm, gate), (up_hbm, up), (down_hbm, down)))
    ]

    def each(do):
        def body(i, carry):
            do(i)
            return carry

        lax.fori_loop(1, half, body, 0)

    pl.semaphore_wait(barrier, half)
    far[PARTS].start()
    far[PARTS + 1].start()
    for c in range(PARTS):
        far[c].start()

    def spread(b, c, masks, source):
        picks = jnp.where(masks[0] | masks[1], 1.0, 0.0).astype(jnp.bfloat16)
        block = slice(b * half * capacity, (b + 1) * half * capacity)
        buffer[block, c * span : (c + 1) * span] = jnp.dot(
            picks, source[:, c * span : (c + 1) * span], preferred_element_type=jnp.float32
        ).astype(jnp.bfloat16)
        each(lambda i: outgoing(b, c, i).start())
        own_in(b, c).start()

    def combines(masks, weights):
        combine = (
            jnp.where(masks[0], weights[0:1, :], 0.0) + jnp.where(masks[1], weights[1:2, :], 0.0)
        ).T
        high = combine.astype(jnp.bfloat16)
        return high, (combine - high.astype(jnp.float32)).astype(jnp.bfloat16)

    def combined(pair, b, c):
        block = returned[
            b * half * capacity : (b + 1) * half * capacity, c * span : (c + 1) * span
        ]
        return jnp.dot(pair[0], block, preferred_element_type=jnp.float32) + jnp.dot(
            pair[1], block, preferred_element_type=jnp.float32
        )

    near_masks = slot_masks(routes_ref[...], base, count, half, capacity)
    for c in range(PARTS):
        spread(0, c, near_masks, xin_ref)
    for load in loads:
        load.start()
    near_pair = combines(near_masks, weights_ref[...])

    far[PARTS].wait_recv()
    far[PARTS + 1].wait_recv()
    far_masks = slot_masks(routes_far[...], base, count, half, capacity)
    far_pair = combines(far_masks, weights_far[...])
    for c in range(PARTS):
        far[c].wait_recv()
        spread(1, c, far_masks, xin_far)
    for load in loads:
        load.wait()

    chunks = 2
    per_chunk = half // chunks
    chunk_rows = per_chunk * capacity
    for b in range(2):
        for c in range(PARTS):
            own_in(b, c).wait()

        def chunk(k, carry, b=b):
            def arrived(i, carry):
                @pl.when(i > 0)
                def _():
                    for c in range(PARTS):
                        outgoing(b, c, i).wait_recv()

                return carry

            lax.fori_loop(k * per_chunk, (k + 1) * per_chunk, arrived, 0)
            start = b * half * capacity + k * chunk_rows
            at = pl.ds(pl.multiple_of(start, chunk_rows), chunk_rows)

            def make_hidden(j, carry):
                cols = pl.ds(pl.multiple_of(j * 256, 256), 256)
                gate_part = jnp.dot(
                    received[at, :], gate[:, cols], preferred_element_type=jnp.float32
                )
                up_part = jnp.dot(received[at, :], up[:, cols], preferred_element_type=jnp.float32)
                hidden[:, cols] = (jax.nn.silu(gate_part) * up_part).astype(jnp.bfloat16)
                return carry

            lax.fori_loop(0, width // 256, make_hidden, 0)

            def make_out(j, carry):
                cols = pl.ds(pl.multiple_of(j * 512, 512), 512)
                results[at, cols] = jnp.dot(
                    hidden[...], down[:, cols], preferred_element_type=jnp.float32
                ).astype(jnp.bfloat16)
                return carry

            lax.fori_loop(0, D // 512, make_out, 0)
            if b == 1:
                for c in range(PARTS):

                    def send_back(i, carry, c=c):
                        @pl.when(i > 0)
                        def _():
                            returning(b, c, i).start()

                        return carry

                    lax.fori_loop(k * per_chunk, (k + 1) * per_chunk, send_back, 0)
            return carry

        lax.fori_loop(0, chunks, chunk, 0)
    for b in (1, 0):
        for c in range(PARTS):
            own_out(b, c).start()
    for c in range(PARTS):
        each(lambda i, c=c: returning(0, c, i).start())

    for c in range(PARTS):
        own_out(1, c).wait()
        each(lambda i, c=c: returning(1, c, i).wait_recv())
        partial[:, c * span : (c + 1) * span] = combined(far_pair, 1, c).astype(jnp.bfloat16)
        far_back[c].start()
    for c in range(PARTS):
        own_out(0, c).wait()
        each(lambda i, c=c: returning(0, c, i).wait_recv())
        near = combined(near_pair, 0, c)
        far_back[c].wait_recv()
        cols = slice(c * span, (c + 1) * span)
        out_ref[:, cols] = (
            mid_ref[:, cols].astype(jnp.float32) + near + far_sum[:, cols].astype(jnp.float32)
        ).astype(jnp.bfloat16)

    for copy in far + far_back:
        copy.wait_send()

    def drain(i):
        for b in range(2):
            for c in range(PARTS):
                outgoing(b, c, i).wait_send()
                returning(b, c, i).wait_send()

    each(drain)


def kernels_on_device(
    residual,
    query_maps,
    key_maps,
    value_rows,
    lambdas,
    head_gain,
    out_weight,
    ffn_gain,
    routes,
    route_weights,
    expert_gate,
    expert_up,
    expert_down,
):
    count_sp = lax.axis_size("sp")
    count_dp = lax.axis_size("dp")
    experts_all = count_sp * count_dp
    rows = residual.shape[1]
    capacity = max(2, 4 * rows // experts_all)
    if capacity % 16 or count_sp % 2:
        return on_device(
            residual,
            query_maps,
            key_maps,
            value_rows,
            lambdas,
            head_gain,
            out_weight,
            ffn_gain,
            routes,
            route_weights,
            expert_gate,
            expert_up,
            expert_down,
        )
    heads_here = HEADS // count_sp
    slots = experts_all * capacity
    vmem = pl.BlockSpec(memory_space=pltpu.VMEM)
    hbm = pl.BlockSpec(memory_space=pl.ANY)
    dma = pltpu.SemaphoreType.DMA
    bf16 = jnp.bfloat16
    length = rows * count_sp
    middle, expert_input = pl.pallas_call(
        functools.partial(mixer_kernel, count_sp),
        out_shape=(
            jax.ShapeDtypeStruct((rows, D), bf16),
            jax.ShapeDtypeStruct((rows, D), bf16),
        ),
        in_specs=[pl.BlockSpec(memory_space=pltpu.SMEM), hbm, hbm, hbm, vmem, vmem, hbm, vmem],
        out_specs=(vmem, vmem),
        scratch_shapes=[
            pltpu.VMEM((heads_here, length, VD), bf16),
            pltpu.VMEM((heads_here, length, VD), bf16),
            pltpu.VMEM((heads_here, length, VD), bf16),
            pltpu.VMEM((heads_here, length, VD), bf16),
            pltpu.VMEM((rows, HEADS * VD), bf16),
            pltpu.VMEM(out_weight.shape, bf16),
            dma((3, heads_here, count_sp)),
            dma((3, heads_here, count_sp)),
            dma((heads_here, count_sp)),
            dma((heads_here, count_sp)),
            dma((3, heads_here)),
            dma,
        ],
        compiler_params=pltpu.CompilerParams(
            collective_id=0, has_side_effects=True, vmem_limit_bytes=VMEM_LIMIT
        ),
    )(
        lambdas,
        query_maps[0],
        key_maps[0],
        value_rows[0],
        residual[0],
        head_gain.reshape(HEADS, VD),
        out_weight,
        ffn_gain.reshape(1, D),
    )
    width = expert_gate.shape[2]
    out = pl.pallas_call(
        functools.partial(experts_kernel, count_sp, count_dp, capacity),
        out_shape=jax.ShapeDtypeStruct((rows, D), bf16),
        in_specs=[vmem, vmem, vmem, vmem, hbm, hbm, hbm],
        out_specs=vmem,
        scratch_shapes=[
            pltpu.VMEM((routes.shape[2], rows), jnp.int32),
            pltpu.VMEM((routes.shape[2], rows), jnp.float32),
            pltpu.VMEM((rows, D), bf16),
            pltpu.VMEM((rows, D), bf16),
            pltpu.VMEM((rows, D), bf16),
            pltpu.VMEM((slots, D), bf16),
            pltpu.VMEM((slots, D), bf16),
            pltpu.VMEM((slots, D), bf16),
            pltpu.VMEM((slots, D), bf16),
            pltpu.VMEM((D, width), bf16),
            pltpu.VMEM((D, width), bf16),
            pltpu.VMEM((width, D), bf16),
            pltpu.VMEM((slots // 4, width), bf16),
            dma((PARTS + 2,)),
            dma((PARTS + 2,)),
            dma((PARTS,)),
            dma((PARTS,)),
            dma((2, PARTS, experts_all // 2)),
            dma((2, PARTS, experts_all // 2)),
            dma((2, PARTS, experts_all // 2)),
            dma((2, PARTS, experts_all // 2)),
            dma((2, 2, PARTS)),
            dma((3,)),
        ],
        compiler_params=pltpu.CompilerParams(
            collective_id=1, has_side_effects=True, vmem_limit_bytes=VMEM_LIMIT
        ),
    )(
        expert_input,
        middle,
        routes[0].T,
        route_weights[0].T,
        expert_gate[0],
        expert_up[0],
        expert_down[0],
    )
    return out[None]


def solution(mesh):
    return jax.shard_map(
        kernels_on_device,
        mesh=mesh,
        in_specs=(
            P("dp", "sp", None),
            P("dp", "sp", None),
            P("dp", "sp", None),
            P("dp", "sp", None),
            P(),
            P(),
            P(),
            P(),
            P("dp", "sp", None),
            P("dp", "sp", None),
            P(("sp", "dp"), None, None),
            P(("sp", "dp"), None, None),
            P(("sp", "dp"), None, None),
        ),
        out_specs=P("dp", "sp", None),
        check_vma=False,
    )
```

```python
import functools
import math

import jax
import jax.numpy as jnp
from jax import lax
from jax.experimental import pallas as pl
from jax.experimental.pallas import tpu as pltpu
from jax.sharding import PartitionSpec as P

D = 2048
HEADS = 16
HD = 64
VD = 128


eps = 1e-06


def attend_head(query_head, key_head, value_head, lam_head, gain_head):
    length = query_head.shape[0]
    block_rows = min(512, length)
    count_blocks = length // block_rows
    scaling = query_head.shape[-1] ** (-0.5)
    query_blocks = query_head.reshape(count_blocks, block_rows, 2, query_head.shape[-1])

    def one_block(query_block):
        scores = (
            jnp.einsum("qmd,kmd->mqk", query_block, key_head, preferred_element_type=jnp.float32)
            * scaling
        )
        probabilities = jax.nn.softmax(scores, axis=-1)
        mixed_map = (probabilities[0] - lam_head * probabilities[1]).astype(jnp.bfloat16)
        head_out = jnp.dot(mixed_map, value_head, preferred_element_type=jnp.float32)
        normed = head_out * lax.rsqrt(jnp.mean(head_out * head_out, axis=-1, keepdims=True) + eps)
        return (normed * gain_head * 0.8).astype(jnp.bfloat16)

    return lax.map(one_block, query_blocks).reshape(length, value_head.shape[-1])


def on_device(
    residual,
    query_maps,
    key_maps,
    value_rows,
    lambdas,
    head_gain,
    out_weight,
    ffn_gain,
    routes,
    route_weights,
    expert_gate,
    expert_up,
    expert_down,
):
    count_sp = lax.axis_size("sp")
    count_dp = lax.axis_size("dp")
    heads_here = HEADS // count_sp
    queries, keys_all, values_all = (
        lax.all_to_all(query_maps, "sp", split_axis=2, concat_axis=1, tiled=True),
        lax.all_to_all(key_maps, "sp", split_axis=2, concat_axis=1, tiled=True),
        lax.all_to_all(value_rows, "sp", split_axis=2, concat_axis=1, tiled=True),
    )
    first_head = lax.axis_index("sp") * heads_here
    lam_here = lax.dynamic_slice_in_dim(lambdas, first_head, heads_here)
    gain_here = lax.dynamic_slice_in_dim(head_gain, first_head * VD, heads_here * VD)
    outputs = []
    for head_index in range(heads_here):
        query_head = queries[0, :, head_index * 2 * HD : (head_index + 1) * 2 * HD].reshape(
            -1, 2, HD
        )
        key_head = keys_all[0, :, head_index * 2 * HD : (head_index + 1) * 2 * HD].reshape(
            -1, 2, HD
        )
        value_head = values_all[0, :, head_index * VD : (head_index + 1) * VD]
        gain_head = gain_here[head_index * VD : (head_index + 1) * VD]
        outputs.append(
            attend_head(query_head, key_head, value_head, lam_here[head_index], gain_head)
        )
    attended = jnp.concatenate(outputs, axis=1)[None]
    returned_heads = lax.all_to_all(attended, "sp", split_axis=1, concat_axis=2, tiled=True)
    projected = jnp.dot(returned_heads[0], out_weight, preferred_element_type=jnp.float32)
    residual_mid = (residual[0].astype(jnp.float32) + projected).astype(jnp.bfloat16)
    middle = residual_mid.astype(jnp.float32)
    expert_input = (
        middle * lax.rsqrt(jnp.mean(middle * middle, axis=-1, keepdims=True) + eps) * ffn_gain
    ).astype(jnp.bfloat16)
    tok_rows = residual.shape[1]
    experts_all = count_sp * count_dp
    capacity = max(2, 4 * tok_rows // experts_all)
    flat_routes = routes[0].reshape(-1)
    flat_weights = route_weights[0].reshape(-1)
    onehot = (flat_routes[:, None] == jnp.arange(experts_all, dtype=jnp.int32)[None, :]).astype(
        jnp.int32
    )
    before = jnp.cumsum(onehot, axis=0) - onehot
    rank_of = jnp.sum(before * onehot, axis=1)
    slot = flat_routes * capacity + rank_of
    token_of = jnp.arange(flat_routes.shape[0], dtype=jnp.int32) // routes.shape[2]
    slot_token = jnp.full((experts_all * capacity,), tok_rows, jnp.int32).at[slot].set(token_of)
    padded_input = jnp.concatenate([expert_input, jnp.zeros((1, D), jnp.bfloat16)], axis=0)
    buffer = padded_input[slot_token].reshape(experts_all, capacity, D)
    received = lax.all_to_all(buffer, ("sp", "dp"), split_axis=0, concat_axis=0, tiled=True)
    row_block = received.reshape(-1, D)
    gate_part = jnp.dot(row_block, expert_gate[0], preferred_element_type=jnp.float32)
    up_part = jnp.dot(row_block, expert_up[0], preferred_element_type=jnp.float32)
    hidden = (jax.nn.silu(gate_part) * up_part).astype(jnp.bfloat16)
    expert_out = jnp.dot(hidden, expert_down[0], preferred_element_type=jnp.float32).astype(
        jnp.bfloat16
    )
    returned = lax.all_to_all(
        expert_out.reshape(received.shape), ("sp", "dp"), split_axis=0, concat_axis=0, tiled=True
    )
    picked = returned.reshape(experts_all * capacity, D)[slot]
    weighted = (picked.astype(jnp.float32) * flat_weights[:, None]).reshape(
        tok_rows, routes.shape[2], D
    )
    layer_out = (middle + jnp.sum(weighted, axis=1)).astype(jnp.bfloat16)
    return layer_out[None]


MESH = pl.DeviceIdType.MESH
VMEM_LIMIT = 60 * 1024 * 1024


def slot_masks(routes, first_expert, experts_all, experts_here, capacity):
    rows = routes.shape[1]
    first, second = routes[0:1, :], routes[1:2, :]
    experts = lax.broadcasted_iota(jnp.int32, (experts_all, rows), 0)
    named_first, named_second = experts == first, experts == second
    named = jnp.where(named_first | named_second, 1.0, 0.0).astype(jnp.bfloat16)
    earlier = lax.broadcasted_iota(jnp.int32, (rows, rows), 0) < lax.broadcasted_iota(
        jnp.int32, (rows, rows), 1
    )
    before = jnp.dot(
        named, jnp.where(earlier, 1.0, 0.0).astype(jnp.bfloat16), preferred_element_type=jnp.float32
    )
    slots = lax.broadcasted_iota(jnp.int32, (experts_here * capacity, rows), 0)
    masks = []
    for route, chosen in ((first, named_first), (second, named_second)):
        rank = jnp.sum(jnp.where(chosen, before, 0.0), axis=0, keepdims=True).astype(jnp.int32)
        masks.append(slots == (route - first_expert) * capacity + rank)
    return masks


def mixer_kernel(
    count_sp,
    lam_ref,
    q_ref,
    k_ref,
    v_ref,
    residual_ref,
    gain_ref,
    ow_hbm,
    fgain_ref,
    mid_ref,
    xin_ref,
    qh,
    kh,
    vh,
    outs,
    att,
    ow,
    send_sem,
    recv_sem,
    back_send,
    back_recv,
    local_sem,
    ow_sem,
):
    me = lax.axis_index("sp")
    rows = q_ref.shape[0]
    heads_here = HEADS // count_sp
    length = rows * count_sp
    sources = ((k_ref, kh), (q_ref, qh), (v_ref, vh))

    barrier = pltpu.get_barrier_semaphore()

    def greet(d, carry):
        pl.semaphore_signal(
            barrier, inc=1, device_id={"sp": lax.rem(me + d, count_sp)}, device_id_type=MESH
        )
        return carry

    lax.fori_loop(1, count_sp, greet, 0)
    weight_copy = pltpu.make_async_copy(ow_hbm, ow, ow_sem)
    my_rows = pl.ds(pl.multiple_of(me * rows, rows), rows)

    def local_copy(t, h):
        src, dst = sources[t]
        cols = pl.ds(pl.multiple_of((me * heads_here + h) * VD, VD), VD)
        return pltpu.make_async_copy(src.at[:, cols], dst.at[h, my_rows, :], local_sem.at[t, h])

    def outgoing(t, h, d):
        src, dst = sources[t]
        peer = lax.rem(me + d, count_sp)
        cols = pl.ds(pl.multiple_of((peer * heads_here + h) * VD, VD), VD)
        return pltpu.make_async_remote_copy(
            src_ref=src.at[:, cols],
            dst_ref=dst.at[h, my_rows, :],
            send_sem=send_sem.at[t, h, d],
            recv_sem=recv_sem.at[t, h, d],
            device_id={"sp": peer},
            device_id_type=MESH,
        )

    pl.semaphore_wait(barrier, count_sp - 1)
    for h in range(heads_here):

        for t in (0, 2, 1):

            def start_all(i, carry, t=t, h=h):
                outgoing(t, h, 1 + lax.rem(i + count_sp // 2 - 1, count_sp - 1)).start()
                return carry

            lax.fori_loop(0, count_sp - 1, start_all, 0)
            local_copy(t, h).start()
    weight_copy.start()

    def returning(h, p, d):
        dst_cols = pl.ds(pl.multiple_of((me * heads_here + h) * VD, VD), VD)
        return pltpu.make_async_remote_copy(
            src_ref=outs.at[h, pl.ds(pl.multiple_of(p * rows, rows), rows), :],
            dst_ref=att.at[:, dst_cols],
            send_sem=back_send.at[h, d],
            recv_sem=back_recv.at[h, d],
            device_id={"sp": p},
            device_id_type=MESH,
        )

    factor = HD ** (-0.5) * math.log2(math.e)
    lanes = lax.broadcasted_iota(jnp.int32, (rows, VD), 1)
    for h in range(heads_here):
        for t in range(3):
            local_copy(t, h).wait()
        for t in (0, 2):

            def arrived(d, carry, t=t, h=h):
                outgoing(t, h, d).wait_recv()
                return carry

            lax.fori_loop(1, count_sp, arrived, 0)
        head = me * heads_here + h
        lam = lam_ref[head]
        gain = gain_ref[pl.ds(head, 1), :]

        def attend(p, h=h, lam=lam, gain=gain):
            at = pl.ds(pl.multiple_of(p * rows, rows), rows)
            q = qh[h, at, :]
            zero = jnp.zeros_like(q)
            both = jnp.concatenate(
                [jnp.where(lanes < HD, q, zero), jnp.where(lanes < HD, zero, q)], axis=0
            )
            scores = lax.dot_general(
                both, kh[h], (((1,), (1,)), ((), ())), preferred_element_type=jnp.float32
            )
            top = jnp.max(scores, axis=1, keepdims=True)
            e = jnp.exp2((scores - top) * factor)
            total = jnp.sum(e, axis=1, keepdims=True)
            total_1, total_2 = total[:rows], total[rows:]
            share = lam * total_1 / total_2
            mixed = (e[:rows] - share * e[rows:]).astype(jnp.bfloat16)
            head_out = jnp.dot(mixed, vh[h], preferred_element_type=jnp.float32) / total_1
            normed = head_out * lax.rsqrt(
                jnp.mean(head_out * head_out, axis=-1, keepdims=True) + eps
            )
            return (normed * gain * 0.8).astype(jnp.bfloat16)

        def step(i, carry, h=h, attend=attend):
            d = 1 + lax.rem(i + count_sp // 2 - 1, count_sp - 1)
            p = lax.rem(me + count_sp - d, count_sp)
            outgoing(1, h, d).wait_recv()
            outs[h, pl.ds(pl.multiple_of(p * rows, rows), rows), :] = attend(p)
            returning(h, p, d).start()
            return carry

        lax.fori_loop(0, count_sp - 1, step, 0)
        att[:, pl.ds(pl.multiple_of(head * VD, VD), VD)] = attend(me)

    weight_copy.wait()
    for h in range(heads_here):

        def back(d, carry, h=h):
            returning(h, lax.rem(me + count_sp - d, count_sp), d).wait_recv()
            return carry

        lax.fori_loop(1, count_sp, back, 0)

    tile = 512
    square = jnp.zeros((rows, 1), jnp.float32)
    for j in range(D // tile):
        cols = slice(j * tile, (j + 1) * tile)
        projected = jnp.dot(att[...], ow[:, cols], preferred_element_type=jnp.float32)
        middle = (residual_ref[:, cols].astype(jnp.float32) + projected).astype(jnp.bfloat16)
        mid_ref[:, cols] = middle
        wide = middle.astype(jnp.float32)
        square = square + jnp.sum(wide * wide, axis=1, keepdims=True)
    scale = lax.rsqrt(square / D + eps)
    xin_ref[...] = (mid_ref[...].astype(jnp.float32) * scale * fgain_ref[...]).astype(jnp.bfloat16)

    for h in range(heads_here):

        def drain(d, carry, h=h):
            for t in range(3):
                outgoing(t, h, d).wait_send()
            returning(h, lax.rem(me + count_sp - d, count_sp), d).wait_send()
            return carry

        lax.fori_loop(1, count_sp, drain, 0)


PARTS = 2


def experts_kernel(
    count_sp,
    count_dp,
    capacity,
    xin_ref,
    mid_ref,
    routes_ref,
    weights_ref,
    gate_hbm,
    up_hbm,
    down_hbm,
    out_ref,
    routes_far,
    weights_far,
    xin_far,
    partial,
    far_sum,
    buffer,
    received,
    results,
    returned,
    gate,
    up,
    down,
    hidden,
    far_send,
    far_recv,
    sum_send,
    sum_recv,
    send_sem,
    recv_sem,
    back_send,
    back_recv,
    own_sem,
    weight_sem,
):
    count = count_sp * count_dp
    half = count // 2
    sp = lax.axis_index("sp")
    base = (sp // (count_sp // 2)) * half
    me = sp * count_dp + lax.axis_index("dp") - base
    partner = {"sp": lax.rem(sp + count_sp // 2, count_sp)}
    width = gate.shape[1]
    span = D // PARTS

    def coords(p):
        return {"sp": (base + p) // count_dp, "dp": lax.rem(base + p, count_dp)}

    barrier = pltpu.get_barrier_semaphore()

    def greet(d, carry):
        pl.semaphore_signal(
            barrier, inc=1, device_id=coords(lax.rem(me + d, half)), device_id_type=MESH
        )
        return carry

    lax.fori_loop(1, half, greet, 0)
    pl.semaphore_signal(barrier, inc=1, device_id=partner, device_id_type=MESH)

    def rows_of(b, i):
        return pl.ds(pl.multiple_of((b * half + i) * capacity, capacity), capacity)

    def part(c):
        return pl.ds(c * span, span)

    def offset(i):
        return 1 + lax.rem(i + half // 2 - 2, half - 1)

    def to_partner(src, dst, sent, got):
        return pltpu.make_async_remote_copy(
            src_ref=src,
            dst_ref=dst,
            send_sem=sent,
            recv_sem=got,
            device_id=partner,
            device_id_type=MESH,
        )

    far = [
        to_partner(xin_ref.at[:, part(c)], xin_far.at[:, part(c)], far_send.at[c], far_recv.at[c])
        for c in range(PARTS)
    ]
    far.append(to_partner(routes_ref, routes_far, far_send.at[PARTS], far_recv.at[PARTS]))
    far.append(
        to_partner(weights_ref, weights_far, far_send.at[PARTS + 1], far_recv.at[PARTS + 1])
    )
    far_back = [
        to_partner(partial.at[:, part(c)], far_sum.at[:, part(c)], sum_send.at[c], sum_recv.at[c])
        for c in range(PARTS)
    ]

    def outgoing(b, c, i):
        p = lax.rem(me + offset(i), half)
        return pltpu.make_async_remote_copy(
            src_ref=buffer.at[rows_of(b, p), part(c)],
            dst_ref=received.at[rows_of(b, i), part(c)],
            send_sem=send_sem.at[b, c, i],
            recv_sem=recv_sem.at[b, c, i],
            device_id=coords(p),
            device_id_type=MESH,
        )

    def returning(b, c, i):
        p = lax.rem(me + half - offset(i), half)
        return pltpu.make_async_remote_copy(
            src_ref=results.at[rows_of(b, i), part(c)],
            dst_ref=returned.at[rows_of(b, me), part(c)],
            send_sem=back_send.at[b, c, i],
            recv_sem=back_recv.at[b, c, i],
            device_id=coords(p),
            device_id_type=MESH,
        )

    def own_in(b, c):
        return pltpu.make_async_copy(
            buffer.at[rows_of(b, me), part(c)],
            received.at[rows_of(b, 0), part(c)],
            own_sem.at[0, b, c],
        )

    def own_out(b, c):
        return pltpu.make_async_copy(
            results.at[rows_of(b, 0), part(c)],
            returned.at[rows_of(b, me), part(c)],
            own_sem.at[1, b, c],
        )

    loads = [
        pltpu.make_async_copy(src, dst, weight_sem.at[j])
        for j, (src, dst) in enumerate(((gate_hbm, gate), (up_hbm, up), (down_hbm, down)))
    ]

    def each(do):
        def body(i, carry):
            do(i)
            return carry

        lax.fori_loop(1, half, body, 0)

    pl.semaphore_wait(barrier, half)
    far[PARTS].start()
    far[PARTS + 1].start()
    for c in range(PARTS):
        far[c].start()

    def spread(b, c, masks, source):
        picks = jnp.where(masks[0] | masks[1], 1.0, 0.0).astype(jnp.bfloat16)
        block = slice(b * half * capacity, (b + 1) * half * capacity)
        buffer[block, c * span : (c + 1) * span] = jnp.dot(
            picks, source[:, c * span : (c + 1) * span], preferred_element_type=jnp.float32
        ).astype(jnp.bfloat16)
        each(lambda i: outgoing(b, c, i).start())
        own_in(b, c).start()

    def combines(masks, weights):
        combine = (
            jnp.where(masks[0], weights[0:1, :], 0.0) + jnp.where(masks[1], weights[1:2, :], 0.0)
        ).T
        high = combine.astype(jnp.bfloat16)
        return high, (combine - high.astype(jnp.float32)).astype(jnp.bfloat16)

    def combined(pair, b, c):
        block = returned[
            b * half * capacity : (b + 1) * half * capacity, c * span : (c + 1) * span
        ]
        return jnp.dot(pair[0], block, preferred_element_type=jnp.float32) + jnp.dot(
            pair[1], block, preferred_element_type=jnp.float32
        )

    near_masks = slot_masks(routes_ref[...], base, count, half, capacity)
    for c in range(PARTS):
        spread(0, c, near_masks, xin_ref)
    for load in loads:
        load.start()
    near_pair = combines(near_masks, weights_ref[...])

    far[PARTS].wait_recv()
    far[PARTS + 1].wait_recv()
    far_masks = slot_masks(routes_far[...], base, count, half, capacity)
    far_pair = combines(far_masks, weights_far[...])
    for c in range(PARTS):
        far[c].wait_recv()
        spread(1, c, far_masks, xin_far)
    for load in loads:
        load.wait()

    for b in range(2):
        at = slice(b * half * capacity, (b + 1) * half * capacity)
        for c in range(PARTS):
            own_in(b, c).wait()
            each(lambda i, b=b, c=c: outgoing(b, c, i).wait_recv())

        def make_hidden(j, carry, at=at):
            cols = pl.ds(pl.multiple_of(j * 256, 256), 256)
            gate_part = jnp.dot(received[at, :], gate[:, cols], preferred_element_type=jnp.float32)
            up_part = jnp.dot(received[at, :], up[:, cols], preferred_element_type=jnp.float32)
            hidden[:, cols] = (jax.nn.silu(gate_part) * up_part).astype(jnp.bfloat16)
            return carry

        lax.fori_loop(0, width // 256, make_hidden, 0)
        for c in range(PARTS):

            def make_out(j, carry, at=at, c=c):
                cols = pl.ds(pl.multiple_of(c * span + j * 512, 512), 512)
                results[at, cols] = jnp.dot(
                    hidden[...], down[:, cols], preferred_element_type=jnp.float32
                ).astype(jnp.bfloat16)
                return carry

            lax.fori_loop(0, span // 512, make_out, 0)
            if b == 1:
                each(lambda i, c=c: returning(1, c, i).start())
    for b in (1, 0):
        for c in range(PARTS):
            own_out(b, c).start()
    for c in range(PARTS):
        each(lambda i, c=c: returning(0, c, i).start())

    for c in range(PARTS):
        own_out(1, c).wait()
        each(lambda i, c=c: returning(1, c, i).wait_recv())
        partial[:, c * span : (c + 1) * span] = combined(far_pair, 1, c).astype(jnp.bfloat16)
        far_back[c].start()
    for c in range(PARTS):
        own_out(0, c).wait()
        each(lambda i, c=c: returning(0, c, i).wait_recv())
        near = combined(near_pair, 0, c)
        far_back[c].wait_recv()
        cols = slice(c * span, (c + 1) * span)
        out_ref[:, cols] = (
            mid_ref[:, cols].astype(jnp.float32) + near + far_sum[:, cols].astype(jnp.float32)
        ).astype(jnp.bfloat16)

    for copy in far + far_back:
        copy.wait_send()

    def drain(i):
        for b in range(2):
            for c in range(PARTS):
                outgoing(b, c, i).wait_send()
                returning(b, c, i).wait_send()

    each(drain)


def kernels_on_device(
    residual,
    query_maps,
    key_maps,
    value_rows,
    lambdas,
    head_gain,
    out_weight,
    ffn_gain,
    routes,
    route_weights,
    expert_gate,
    expert_up,
    expert_down,
):
    count_sp = lax.axis_size("sp")
    count_dp = lax.axis_size("dp")
    experts_all = count_sp * count_dp
    rows = residual.shape[1]
    capacity = max(2, 4 * rows // experts_all)
    if capacity % 16 or count_sp % 2:
        return on_device(
            residual,
            query_maps,
            key_maps,
            value_rows,
            lambdas,
            head_gain,
            out_weight,
            ffn_gain,
            routes,
            route_weights,
            expert_gate,
            expert_up,
            expert_down,
        )
    heads_here = HEADS // count_sp
    slots = experts_all * capacity
    vmem = pl.BlockSpec(memory_space=pltpu.VMEM)
    hbm = pl.BlockSpec(memory_space=pl.ANY)
    dma = pltpu.SemaphoreType.DMA
    bf16 = jnp.bfloat16
    length = rows * count_sp
    middle, expert_input = pl.pallas_call(
        functools.partial(mixer_kernel, count_sp),
        out_shape=(
            jax.ShapeDtypeStruct((rows, D), bf16),
            jax.ShapeDtypeStruct((rows, D), bf16),
        ),
        in_specs=[pl.BlockSpec(memory_space=pltpu.SMEM), hbm, hbm, hbm, vmem, vmem, hbm, vmem],
        out_specs=(vmem, vmem),
        scratch_shapes=[
            pltpu.VMEM((heads_here, length, VD), bf16),
            pltpu.VMEM((heads_here, length, VD), bf16),
            pltpu.VMEM((heads_here, length, VD), bf16),
            pltpu.VMEM((heads_here, length, VD), bf16),
            pltpu.VMEM((rows, HEADS * VD), bf16),
            pltpu.VMEM(out_weight.shape, bf16),
            dma((3, heads_here, count_sp)),
            dma((3, heads_here, count_sp)),
            dma((heads_here, count_sp)),
            dma((heads_here, count_sp)),
            dma((3, heads_here)),
            dma,
        ],
        compiler_params=pltpu.CompilerParams(
            collective_id=0, has_side_effects=True, vmem_limit_bytes=VMEM_LIMIT
        ),
    )(
        lambdas,
        query_maps[0],
        key_maps[0],
        value_rows[0],
        residual[0],
        head_gain.reshape(HEADS, VD),
        out_weight,
        ffn_gain.reshape(1, D),
    )
    width = expert_gate.shape[2]
    out = pl.pallas_call(
        functools.partial(experts_kernel, count_sp, count_dp, capacity),
        out_shape=jax.ShapeDtypeStruct((rows, D), bf16),
        in_specs=[vmem, vmem, vmem, vmem, hbm, hbm, hbm],
        out_specs=vmem,
        scratch_shapes=[
            pltpu.VMEM((routes.shape[2], rows), jnp.int32),
            pltpu.VMEM((routes.shape[2], rows), jnp.float32),
            pltpu.VMEM((rows, D), bf16),
            pltpu.VMEM((rows, D), bf16),
            pltpu.VMEM((rows, D), bf16),
            pltpu.VMEM((slots, D), bf16),
            pltpu.VMEM((slots, D), bf16),
            pltpu.VMEM((slots, D), bf16),
            pltpu.VMEM((slots, D), bf16),
            pltpu.VMEM((D, width), bf16),
            pltpu.VMEM((D, width), bf16),
            pltpu.VMEM((width, D), bf16),
            pltpu.VMEM((slots // 2, width), bf16),
            dma((PARTS + 2,)),
            dma((PARTS + 2,)),
            dma((PARTS,)),
            dma((PARTS,)),
            dma((2, PARTS, experts_all // 2)),
            dma((2, PARTS, experts_all // 2)),
            dma((2, PARTS, experts_all // 2)),
            dma((2, PARTS, experts_all // 2)),
            dma((2, 2, PARTS)),
            dma((3,)),
        ],
        compiler_params=pltpu.CompilerParams(
            collective_id=1, has_side_effects=True, vmem_limit_bytes=VMEM_LIMIT
        ),
    )(
        expert_input,
        middle,
        routes[0].T,
        route_weights[0].T,
        expert_gate[0],
        expert_up[0],
        expert_down[0],
    )
    return out[None]


def solution(mesh):
    return jax.shard_map(
        kernels_on_device,
        mesh=mesh,
        in_specs=(
            P("dp", "sp", None),
            P("dp", "sp", None),
            P("dp", "sp", None),
            P("dp", "sp", None),
            P(),
            P(),
            P(),
            P(),
            P("dp", "sp", None),
            P("dp", "sp", None),
            P(("sp", "dp"), None, None),
            P(("sp", "dp"), None, None),
            P(("sp", "dp"), None, None),
        ),
        out_specs=P("dp", "sp", None),
        check_vma=False,
    )
```
